32 devices in a mesh: ep: 8 (over z, x), tp: 4 (over y, core).
Axes of the slice: x: 2, y: 2, z: 4, core: 2. Of those that a mesh axis runs over, the one named last changes fastest.
Arguments:
- hidden_in: bfloat16 [128, 4096], P('ep'), may hold values from -6 to 6
- w_query: bfloat16 [4096, 2048], P('ep', 'tp'), may hold values from -0.09375 to 0.09375
- w_key: bfloat16 [4096, 2048], P('ep', 'tp'), may hold values from -0.09375 to 0.09375
- w_value: bfloat16 [4096, 2048], P('ep', 'tp'), may hold values from -0.09375 to 0.09375
- w_outgate: bfloat16 [4096, 2048], P('ep', 'tp'), may hold values from -0.09375 to 0.09375
- w_igate: bfloat16 [4096, 16], P('ep', 'tp'), may hold values from -0.09375 to 0.09375
- w_fgate: bfloat16 [4096, 16], P('ep', 'tp'), may hold values from -0.09375 to 0.09375
- input_bias: float32 [16], P('tp'), may hold values from -3 to 303
- forget_bias: float32 [16], P('tp'), may hold values from -1 to 5
- mem_state: float32 [128, 16, 16384], P('ep', 'tp'), may hold values from -4 to 4
- max_state: float32 [128, 16], P('ep', 'tp'), may hold values from -4 to 304
- head_gain: float32 [2048], P('tp'), may hold values from 0.1 to 1.9
- w_output: bfloat16 [2048, 4096], P('tp'), may hold values from -0.26367188 to 0.26367188
- first_gain: float32 [4096], replicated, may hold values from 0.35 to 3.25
- w_group_router: bfloat16 [4096, 2], replicated, may hold values from -0.09375 to 0.09375
- w_expert_router: bfloat16 [4096, 8], replicated, may hold values from -0.09375 to 0.09375
- expert_route: int32 [128, 2], P('ep'), may hold values from 0 to 7, as said below
- w_expgate: bfloat16 [8, 4096, 1024], P('ep', None, 'tp'), may hold values from -0.09375 to 0.09375
- w_expup: bfloat16 [8, 4096, 1024], P('ep', None, 'tp'), may hold values from -0.09375 to 0.09375
- w_expdown: bfloat16 [8, 1024, 4096], P('ep', 'tp'), may hold values from -0.75 to 0.75
- second_gain: float32 [4096], P('tp'), may hold values from 0.1 to 1.9
Outputs:
- hidden_out: bfloat16 [128, 4096], P('ep', 'tp')
- mem_next: float32 [128, 16, 16384], P('ep', 'tp')
- max_next: float32 [128, 16], P('ep', 'tp')
The draws below stay inside these ranges and needn't reach their ends.
Inputs may be any that keep to these rules, and one draw needn't show every extreme that they name: `expert_route`: each row names two different experts of one group (an expert's group is its number divided by 4). In each aligned block of 16 rows (the rows of one index of ep) every group is named by exactly 8 rows, no expert by more than 8 rows, and some expert by exactly 8 rows.
All inputs are finite; a program needn't handle non-finite values.
Results may differ from the reference program's by a relative error of at most 0.02.
Values may be sent and summed in bfloat16 or wider, within the bound.
A program may use at most 64 MiB of HBM per device.

```python
import jax
import jax.numpy as jnp
from jax import lax

D = 4096
HEADS = 16
DH = 128
HD = 2048
DE = 1024
GROUP_SIZE = 4
TOP_K = 2
EXPERTS = 8
GROUPS = 2
SEQ_DEV = 16
SEQUENCES = 128
CAP = 8
N_EP = 8
N_TP = 4


def draw_input_bias(key, part):
    base = jax.random.uniform(jax.random.fold_in(key, 1), (HEADS,), jnp.float32, -3.0, 3.0)
    return base


def draw_max_state(key, part):
    base = jax.random.uniform(jax.random.fold_in(key, 2), (SEQUENCES, HEADS), jnp.float32, -4.0, 4.0)
    return base


def draw_first_gain(key, part):
    positions = jnp.arange(D, dtype=jnp.float32) / D
    rough = jax.random.uniform(jax.random.fold_in(key, 3), (D,), jnp.float32, 0.7, 1.3)
    ramp = 0.5 * jnp.power(5.0, positions)
    return ramp * rough


def route_block(block_key):
    coin_key, forced_key, perm_key, swap_key, order_key = jax.random.split(block_key, 5)
    skewed = jax.random.randint(coin_key, (GROUPS,), 0, 2)
    forced = jax.random.randint(forced_key, (), 0, GROUPS)
    skewed = jnp.where(jnp.arange(GROUPS) == forced, 1, skewed)
    ranks_to_expert = jax.vmap(lambda one_key: jax.random.permutation(one_key, GROUP_SIZE))(jax.random.split(perm_key, GROUPS))
    skew_counts = jnp.array([CAP, 0, CAP // 2, CAP // 2], jnp.int32)
    even_counts = jnp.array([CAP // 2, CAP // 2, CAP // 2, CAP // 2], jnp.int32)
    counts = jnp.where(skewed[:, None] == 1, skew_counts[None, :], even_counts[None, :])
    running = jnp.cumsum(counts, 1)
    slots = jnp.arange(2 * CAP, dtype=jnp.int32)
    rank_of_slot = jnp.sum((slots[None, :, None] >= running[:, None, :]).astype(jnp.int32), -1)
    expert_of_slot = jnp.take_along_axis(ranks_to_expert, rank_of_slot, 1) + GROUP_SIZE * jnp.arange(GROUPS, dtype=jnp.int32)[:, None]
    pairs = jnp.stack([expert_of_slot[:, :CAP], expert_of_slot[:, CAP:]], -1).reshape(GROUPS * CAP, 2)
    swapped = jax.random.randint(swap_key, (GROUPS * CAP,), 0, 2)
    pairs = jnp.where(swapped[:, None] == 1, pairs[:, ::-1], pairs)
    order = jax.random.permutation(order_key, GROUPS * CAP)
    return pairs[order]


def draw_expert_route(key, part):
    block_keys = jax.random.split(jax.random.fold_in(key, 5), SEQUENCES // SEQ_DEV)
    routes = jax.vmap(route_block)(block_keys)
    return routes.reshape(SEQUENCES, TOP_K).astype(jnp.int32)


def shard_levels(rng, dims, cuts, least, largest):
    def one(position, parts):
        heights = jax.random.uniform(jax.random.fold_in(jax.random.fold_in(rng, 6), position), (parts,), jnp.float32, least / len(cuts), largest / len(cuts))
        return jnp.repeat(jnp.exp(heights), dims[position] // parts).reshape((-1,) + (1,) * (len(dims) - position - 1))

    level = one(*cuts[0])
    for cut in cuts[1:]:
        level = level * one(*cut)
    return level


def bell_draw(key, shape, deviation, reach, cuts=(), held_as=jnp.bfloat16):
    drawn = jax.random.normal(key, shape, jnp.float32) * deviation
    if len(cuts) > 0:
        drawn = shard_levels(key, shape, cuts, -0.22, 0.18) * drawn
    return jnp.clip(drawn, min=-reach, max=reach).astype(held_as)


def setup_inputs(seed: int = 0) -> dict:
    streams_of = jax.random.split(jax.random.key(seed), 22)
    return {
        "hidden_in": bell_draw(streams_of[0], (SEQUENCES, D), 1.0, 6.0, ((0, 8),)),
        "w_query": bell_draw(streams_of[1], (D, HD), D ** -0.5, 0.09375, ((0, 8), (1, 4))),
        "w_key": bell_draw(streams_of[2], (D, HD), D ** -0.5, 0.09375, ((0, 8), (1, 4))),
        "w_value": bell_draw(streams_of[3], (D, HD), D ** -0.5, 0.09375, ((0, 8), (1, 4))),
        "w_outgate": bell_draw(streams_of[4], (D, HD), D ** -0.5, 0.09375, ((0, 8), (1, 4))),
        "w_igate": bell_draw(streams_of[5], (D, HEADS), D ** -0.5, 0.09375, ((0, 8), (1, 4))),
        "w_fgate": bell_draw(streams_of[6], (D, HEADS), D ** -0.5, 0.09375, ((0, 8), (1, 4))),
        "input_bias": draw_input_bias(jax.random.fold_in(streams_of[21], 71), 0),
        "forget_bias": jnp.clip(-1.0 + 6.0 * jax.random.uniform(streams_of[8], (HEADS,), jnp.float32) ** shard_levels(streams_of[8], (HEADS,), ((0, 4),), -0.2, 0.2), -1.0, 5.0),
        "mem_state": bell_draw(streams_of[9], (SEQUENCES, HEADS, DH * DH), 0.5, 4.0, ((0, 8), (1, 4)), jnp.float32),
        "max_state": draw_max_state(jax.random.fold_in(streams_of[21], 71), 0),
        "head_gain": jnp.clip(1.0 + 0.18 * jax.random.normal(streams_of[11], (HD,), jnp.float32), 0.1, 1.9),
        "w_output": bell_draw(streams_of[12], (HD, D), (2.0 / HD ** 0.5), 0.26367188, ((0, 4),)),
        "first_gain": draw_first_gain(jax.random.fold_in(streams_of[21], 71), 0),
        "w_group_router": bell_draw(streams_of[14], (D, GROUPS), D ** -0.5, 0.09375),
        "w_expert_router": bell_draw(streams_of[15], (D, EXPERTS), D ** -0.5, 0.09375),
        "expert_route": draw_expert_route(jax.random.fold_in(streams_of[21], 71), 0),
        "w_expgate": bell_draw(streams_of[17], (EXPERTS, D, DE), D ** -0.5, 0.09375, ((0, 8), (2, 4))),
        "w_expup": bell_draw(streams_of[18], (EXPERTS, D, DE), D ** -0.5, 0.09375, ((0, 8), (2, 4))),
        "w_expdown": bell_draw(streams_of[19], (EXPERTS, DE, D), (4.0 / DE ** 0.5), 0.75, ((0, 8), (1, 4))),
        "second_gain": jnp.clip(1.0 + 0.18 * jax.random.normal(streams_of[20], (D,), jnp.float32), 0.1, 1.9),
    }


res_alpha = 8.0 ** 0.25

def layer_norm(values, gain):
    row_mean = lax.optimization_barrier(jnp.mean(values, -1, keepdims=True))
    row_var = lax.optimization_barrier(jnp.mean(values * values, -1, keepdims=True)) - row_mean * row_mean
    return (values - row_mean) * lax.rsqrt(row_var + 1e-05) * gain

def mlstm_step(queries, keys_scaled, values, log_input, log_forget, memory, stabilizer):
    new_max = jnp.maximum(log_forget + stabilizer, log_input)
    keep_old = jnp.exp(log_forget + stabilizer - new_max)
    write_new = jnp.exp(log_input - new_max)
    scores = lax.optimization_barrier(jnp.sum(queries * keys_scaled, -1)) * write_new
    read_old = jnp.einsum('bhd,bhde->bhe', queries, memory, precision=lax.Precision.HIGHEST)
    readout = scores[..., None] * values + keep_old[..., None] * read_old
    memory_next = keep_old[..., None, None] * memory + write_new[..., None, None] * keys_scaled[..., :, None] * values[..., None, :]
    return (readout, memory_next, new_max)

def head_mix(readout, head_gain, out_pre):
    scaled = readout * lax.rsqrt(lax.optimization_barrier(jnp.mean(readout * readout, -1, keepdims=True)) + 1e-06)
    flat_heads = scaled.reshape(scaled.shape[0], -1)
    return (flat_heads * head_gain * jax.nn.sigmoid(out_pre)).astype(jnp.bfloat16)

def route_weights(mid_float, w_group_router, w_expert_router, expert_route):
    group_logits = jnp.dot(mid_float, w_group_router.astype(jnp.float32), precision=lax.Precision.HIGHEST)
    expert_logits = jnp.dot(mid_float, w_expert_router.astype(jnp.float32), precision=lax.Precision.HIGHEST)
    first_expert = expert_route[:, 0]
    second_expert = expert_route[:, 1]
    expert_ids = lax.broadcasted_iota(jnp.int32, expert_logits.shape, 1)
    group_ids = lax.broadcasted_iota(jnp.int32, group_logits.shape, 1)
    first_logit = lax.optimization_barrier(jnp.sum(jnp.where(expert_ids == first_expert[:, None], expert_logits, 0.0), -1))
    second_logit = lax.optimization_barrier(jnp.sum(jnp.where(expert_ids == second_expert[:, None], expert_logits, 0.0), -1))
    group_pick = lax.optimization_barrier(jnp.sum(jnp.where(group_ids == (first_expert // GROUP_SIZE)[:, None], group_logits, 0.0), -1))
    group_gate = jax.nn.sigmoid(group_pick)
    return (group_gate * jax.nn.sigmoid(first_logit - second_logit), group_gate * jax.nn.sigmoid(second_logit - first_logit))

def slot_ranks(flat_routes, expert_total):
    onehot = (flat_routes[:, None] == lax.broadcasted_iota(jnp.int32, (flat_routes.shape[0], expert_total), 1)).astype(jnp.int32)
    running = jnp.cumsum(onehot, 0)
    return lax.optimization_barrier(jnp.sum((running - 1) * onehot, -1)).astype(jnp.int32)

def add_block(total, pieces):
    block_rows, block_weight = pieces
    partial_sum = jnp.dot(block_rows, block_weight, preferred_element_type=jnp.float32)
    partial_sum = lax.optimization_barrier(partial_sum.astype(jnp.bfloat16)).astype(jnp.float32)
    return (total + partial_sum, None)

def blocked_product(left, right):
    row_count = left.shape[0]
    inner = left.shape[1] // N_TP
    left_blocks = left.reshape(row_count, N_TP, inner).transpose(1, 0, 2)
    right_blocks = right.reshape(N_TP, inner, right.shape[1])
    total, unused = lax.scan(add_block, jnp.zeros((row_count, right.shape[1]), jnp.float32), (left_blocks, right_blocks))
    return total

def run_expert(pieces):
    rows_in, gate_weight, up_weight, down_weight = pieces
    gate_pre = jnp.dot(rows_in, gate_weight, preferred_element_type=jnp.float32)
    up_pre = jnp.dot(rows_in, up_weight, preferred_element_type=jnp.float32)
    hidden_units = (jax.nn.silu(gate_pre) * up_pre).astype(jnp.bfloat16)
    return blocked_product(hidden_units, down_weight).astype(jnp.bfloat16)

def reference(hidden_in, w_query, w_key, w_value, w_outgate, w_igate, w_fgate, input_bias, forget_bias, mem_state, max_state, head_gain, w_output, first_gain, w_group_router, w_expert_router, expert_route, w_expgate, w_expup, w_expdown, second_gain):
    shape4 = (SEQUENCES, HEADS, DH)
    queries = jnp.dot(hidden_in, w_query, preferred_element_type=jnp.float32).reshape(shape4)
    keys_scaled = jnp.dot(hidden_in, w_key, preferred_element_type=jnp.float32).reshape(shape4) * DH ** (-0.5)
    values = jnp.dot(hidden_in, w_value, preferred_element_type=jnp.float32).reshape(shape4)
    out_pre = jnp.dot(hidden_in, w_outgate, preferred_element_type=jnp.float32)
    log_input = jnp.dot(hidden_in, w_igate, preferred_element_type=jnp.float32) + input_bias
    log_forget = jax.nn.log_sigmoid(jnp.dot(hidden_in, w_fgate, preferred_element_type=jnp.float32) + forget_bias)
    memory = mem_state.reshape(SEQUENCES, HEADS, DH, DH)
    readout, mem_square, max_next = mlstm_step(queries, keys_scaled, values, log_input, log_forget, memory, max_state)
    mem_next = mem_square.reshape(SEQUENCES, HEADS, DH * DH)
    mixed_heads = head_mix(readout, head_gain, out_pre)
    mix = blocked_product(mixed_heads, w_output)
    mid_float = layer_norm(res_alpha * hidden_in.astype(jnp.float32) + mix, first_gain)
    mid = mid_float.astype(jnp.bfloat16)
    first_weight, second_weight = route_weights(mid_float, w_group_router, w_expert_router, expert_route)
    flat_routes = expert_route.reshape(-1).astype(jnp.int32)
    block_routes = flat_routes.reshape(N_EP, TOP_K * SEQ_DEV)
    ranks = jax.vmap(slot_ranks, in_axes=(0, None))(block_routes, EXPERTS).reshape(-1)
    source_block = (jnp.arange(SEQUENCES * TOP_K, dtype=jnp.int32) // (TOP_K * SEQ_DEV)).astype(jnp.int32)
    slot_index = ((flat_routes * N_EP + source_block) * CAP + ranks).astype(jnp.int32)
    repeated = jnp.repeat(mid, TOP_K, 0)
    buffer = jnp.zeros((EXPERTS * N_EP * CAP, D), jnp.bfloat16).at[slot_index].set(repeated)
    buffer = buffer.reshape(EXPERTS, N_EP * CAP, D)
    expert_out = lax.map(run_expert, (buffer, w_expgate, w_expup, w_expdown)).reshape(EXPERTS * N_EP * CAP, D)
    picked = expert_out[slot_index].astype(jnp.float32).reshape(SEQUENCES, TOP_K, D)
    moe = first_weight[:, None] * picked[:, 0] + second_weight[:, None] * picked[:, 1]
    joined = res_alpha * mid.astype(jnp.float32) + moe
    hidden_out = layer_norm(joined, second_gain).astype(jnp.bfloat16)
    return (hidden_out, mem_next, max_next)
```

```python
import functools

import jax
import jax.numpy as jnp
from jax import lax
from jax.experimental import pallas as pl
from jax.experimental.pallas import tpu as pltpu
from jax.sharding import PartitionSpec as P

D = 4096
DH = 128
GROUP_SIZE = 4
MESH = pl.DeviceIdType.MESH


res_alpha = 8.0**0.25


def layer_norm(values, gain):
    row_mean = jnp.mean(values, -1, keepdims=True)
    row_var = jnp.mean(values * values, -1, keepdims=True) - row_mean * row_mean
    return (values - row_mean) * lax.rsqrt(row_var + 1e-05) * gain


def mlstm_step(queries, keys_scaled, values, log_input, log_forget, memory, stabilizer):
    new_max = jnp.maximum(log_forget + stabilizer, log_input)
    keep_old = jnp.exp(log_forget + stabilizer - new_max)
    write_new = jnp.exp(log_input - new_max)
    scores = jnp.sum(queries * keys_scaled, -1) * write_new
    read_old = jnp.einsum("bhd,bhde->bhe", queries, memory, precision=lax.Precision.HIGHEST)
    readout = scores[..., None] * values + keep_old[..., None] * read_old
    memory_next = (
        keep_old[..., None, None] * memory
        + write_new[..., None, None] * keys_scaled[..., :, None] * values[..., None, :]
    )
    return (readout, memory_next, new_max)


def head_mix(readout, head_gain, out_pre):
    scaled = readout * lax.rsqrt(jnp.mean(readout * readout, -1, keepdims=True) + 1e-06)
    flat_heads = scaled.reshape(scaled.shape[0], -1)
    return (flat_heads * head_gain * jax.nn.sigmoid(out_pre)).astype(jnp.bfloat16)


def route_weights(mid_float, w_group_router, w_expert_router, expert_route):
    group_logits = jnp.dot(
        mid_float, w_group_router.astype(jnp.float32), precision=lax.Precision.HIGHEST
    )
    expert_logits = jnp.dot(
        mid_float, w_expert_router.astype(jnp.float32), precision=lax.Precision.HIGHEST
    )
    first_expert = expert_route[:, 0]
    second_expert = expert_route[:, 1]
    expert_ids = lax.broadcasted_iota(jnp.int32, expert_logits.shape, 1)
    group_ids = lax.broadcasted_iota(jnp.int32, group_logits.shape, 1)
    first_logit = jnp.sum(jnp.where(expert_ids == first_expert[:, None], expert_logits, 0.0), -1)
    second_logit = jnp.sum(jnp.where(expert_ids == second_expert[:, None], expert_logits, 0.0), -1)
    group_pick = jnp.sum(
        jnp.where(group_ids == (first_expert // GROUP_SIZE)[:, None], group_logits, 0.0), -1
    )
    group_gate = jax.nn.sigmoid(group_pick)
    return (
        group_gate * jax.nn.sigmoid(first_logit - second_logit),
        group_gate * jax.nn.sigmoid(second_logit - first_logit),
    )


def slot_ranks(flat_routes, expert_total):
    onehot = (
        flat_routes[:, None]
        == lax.broadcasted_iota(jnp.int32, (flat_routes.shape[0], expert_total), 1)
    ).astype(jnp.int32)
    running = jnp.cumsum(onehot, 0)
    return jnp.sum((running - 1) * onehot, -1)


def body(
    hidden_in,
    w_query,
    w_key,
    w_value,
    w_outgate,
    w_igate,
    w_fgate,
    input_bias,
    forget_bias,
    mem_state,
    max_state,
    head_gain,
    w_output,
    first_gain,
    w_group_router,
    w_expert_router,
    expert_route,
    w_expgate,
    w_expup,
    w_expdown,
    second_gain,
):
    own_rows, width = hidden_in.shape
    heads_here = mem_state.shape[1]
    head_width = heads_here * DH
    top_count = expert_route.shape[1]
    spread_rows = lax.all_to_all(hidden_in, "ep", split_axis=1, concat_axis=0, tiled=True)
    stacked_w = jnp.concatenate([w_query, w_key, w_value, w_outgate], 1)
    gate_w = jnp.concatenate([w_igate, w_fgate], 1)
    proj_terms = jnp.dot(spread_rows, stacked_w, preferred_element_type=jnp.float32)
    gate_terms = jnp.dot(spread_rows, gate_w, preferred_element_type=jnp.float32)
    projected, gate_sums = (
        lax.psum_scatter(proj_terms, "ep", scatter_dimension=0, tiled=True),
        lax.psum_scatter(gate_terms, "ep", scatter_dimension=0, tiled=True),
    )
    shaped = projected.reshape(own_rows, 4, heads_here, DH)
    queries = shaped[:, 0]
    keys_raw = shaped[:, 1]
    values = shaped[:, 2]
    out_pre = shaped[:, 3].reshape(own_rows, head_width)
    input_sum = gate_sums[:, :heads_here]
    forget_sum = gate_sums[:, heads_here:]
    keys_scaled = keys_raw * DH ** (-0.5)
    log_input = input_sum + input_bias
    log_forget = jax.nn.log_sigmoid(forget_sum + forget_bias)
    memory = mem_state.reshape(own_rows, heads_here, DH, DH)
    readout, memory_square, new_max = mlstm_step(
        queries, keys_scaled, values, log_input, log_forget, memory, max_state
    )
    memory_next = memory_square.reshape(own_rows, heads_here, DH * DH)
    mixed_heads = head_mix(readout, head_gain, out_pre)
    partial_mix = jnp.dot(mixed_heads, w_output, preferred_element_type=jnp.float32).astype(
        jnp.bfloat16
    )
    mix = lax.psum(partial_mix.astype(jnp.float32).astype(jnp.bfloat16), "tp").astype(jnp.float32)
    mid_float = layer_norm(res_alpha * hidden_in.astype(jnp.float32) + mix, first_gain)
    mid = mid_float.astype(jnp.bfloat16)
    first_weight, second_weight = route_weights(
        mid_float, w_group_router, w_expert_router, expert_route
    )
    expert_total = w_expgate.shape[0] * lax.axis_size("ep")
    capacity = 2 * own_rows * top_count // expert_total
    flat_routes = expert_route.reshape(-1)
    local_slot = flat_routes * capacity + slot_ranks(flat_routes, expert_total)
    share_width = width // lax.axis_size("tp")
    mid_share = lax.dynamic_slice_in_dim(mid, lax.axis_index("tp") * share_width, share_width, 1)
    buffer = (
        jnp.zeros((expert_total * capacity, width), jnp.bfloat16)
        .at[local_slot]
        .set(jnp.repeat(mid, top_count, 0))
    )
    arrived = lax.all_to_all(
        buffer.reshape(expert_total, capacity, width), "ep", split_axis=0, concat_axis=1, tiled=True
    )
    gate_pre = jnp.einsum("erd,edf->erf", arrived, w_expgate, preferred_element_type=jnp.float32)
    up_pre = jnp.einsum("erd,edf->erf", arrived, w_expup, preferred_element_type=jnp.float32)
    hidden_units = (jax.nn.silu(gate_pre) * up_pre).astype(jnp.bfloat16)
    down_terms = jnp.einsum(
        "erf,efd->erd", hidden_units, w_expdown, preferred_element_type=jnp.float32
    ).astype(jnp.bfloat16)
    expert_share = lax.psum_scatter(
        down_terms.astype(jnp.float32).astype(jnp.bfloat16), "tp", scatter_dimension=2, tiled=True
    )
    returned = lax.all_to_all(expert_share, "ep", split_axis=1, concat_axis=0, tiled=True)
    picked = returned.reshape(expert_total * capacity, share_width)[local_slot]
    picked = picked.astype(jnp.float32).reshape(own_rows, top_count, share_width)
    moe = first_weight[:, None] * picked[:, 0] + second_weight[:, None] * picked[:, 1]
    joined = res_alpha * mid_share.astype(jnp.float32) + moe
    row_sum, square_sum = lax.psum((jnp.sum(joined, -1), jnp.sum(joined * joined, -1)), "tp")
    row_mean = row_sum / D
    row_var = square_sum / D - row_mean * row_mean
    hidden_out = (
        (joined - row_mean[:, None]) * lax.rsqrt(row_var[:, None] + 1e-05) * second_gain
    ).astype(jnp.bfloat16)
    return (hidden_out, memory_next, new_max)


def greet(peers):
    barrier = pltpu.get_barrier_semaphore()
    for peer in peers:
        pl.semaphore_signal(barrier, inc=1, device_id=peer, device_id_type=MESH)
    pl.semaphore_wait(barrier, len(peers))


def remote(source, target, send_sem, recv_sem, peer):
    return pltpu.make_async_remote_copy(
        src_ref=source,
        dst_ref=target,
        send_sem=send_sem,
        recv_sem=recv_sem,
        device_id=peer,
        device_id_type=MESH,
    )


def project_kernel(
    n_ep,
    hidden,
    gate_w,
    wq,
    wk,
    wv,
    wo,
    proj_out,
    gate_out,
    weights,
    spread,
    half_send,
    half_recv,
    full_send,
    full_recv,
    gate_send,
    gate_recv,
    load_sem,
    h_send,
    h_recv,
    v_send,
    v_recv,
    q_send,
    q_recv,
    g_send,
    g_recv,
):
    me = lax.axis_index("ep")
    tp = lax.axis_index("tp")
    rows = hidden.shape[0]
    depth, cols = wq.shape
    loads = [pltpu.make_async_copy(w, weights.at[i], load_sem.at[i]) for i, w in enumerate((wq, wk, wv, wo))]
    for load in loads:
        load.start()
    after = [(lax.rem(me + o, n_ep), tp) for o in range(n_ep)]
    before = [(lax.rem(me + n_ep - o, n_ep), tp) for o in range(n_ep)]
    greet(after[1:])
    sent = []
    for o in range(1, n_ep):
        columns = pl.ds(pl.multiple_of(after[o][0] * depth, depth), depth)
        copy = remote(hidden.at[:, columns], spread.at[o], h_send.at[o], h_recv.at[o], after[o])
        copy.start()
        sent.append(copy)
    spread[0] = hidden[:, pl.ds(pl.multiple_of(me * depth, depth), depth)]
    for load in loads:
        load.wait()
    for copy in sent:
        copy.wait_recv()
    lhs = spread[...].reshape(n_ep * rows, depth)
    gates = jnp.dot(lhs, gate_w[...], preferred_element_type=jnp.float32)
    gate_send[...] = gates.reshape(n_ep, rows, gates.shape[1])
    gate_copies = [remote(gate_send.at[o], gate_recv.at[o], g_send.at[o], g_recv.at[o], before[o]) for o in range(1, n_ep)]
    for copy in gate_copies:
        copy.start()
    for i in range(2):
        part = jnp.dot(lhs, weights[2 + i], preferred_element_type=jnp.float32)
        half_send[:, :, i * cols : (i + 1) * cols] = part.astype(jnp.bfloat16).reshape(n_ep, rows, cols)
    half_copies = [remote(half_send.at[o], half_recv.at[o], v_send.at[o], v_recv.at[o], before[o]) for o in range(1, n_ep)]
    for copy in half_copies:
        copy.start()
    for i in range(2):
        part = jnp.dot(lhs, weights[i], preferred_element_type=jnp.float32)
        full_send[:, :, i * cols : (i + 1) * cols] = part.reshape(n_ep, rows, cols)
    full_copies = [remote(full_send.at[o], full_recv.at[o], q_send.at[o], q_recv.at[o], before[o]) for o in range(1, n_ep)]
    for copy in full_copies:
        copy.start()
    gate_total = gate_send[0]
    half_part = slice(2 * cols, 4 * cols)
    full_part = slice(0, 2 * cols)
    proj_out[:, half_part] = half_send[0].astype(jnp.float32)
    proj_out[:, full_part] = full_send[0]
    for o in range(1, n_ep):
        gate_copies[o - 1].wait_recv()
        gate_total += gate_recv[o]
        half_copies[o - 1].wait_recv()
        proj_out[:, half_part] += half_recv[o].astype(jnp.float32)
    for o in range(1, n_ep):
        full_copies[o - 1].wait_recv()
        proj_out[:, full_part] += full_recv[o]
    gate_out[...] = gate_total
    for copy in sent + gate_copies + half_copies + full_copies:
        copy.wait_send()


def project(n_ep, hidden, gate_w, wq, wk, wv, wo):
    rows = hidden.shape[0]
    depth, cols = wq.shape
    vmem = pl.BlockSpec(memory_space=pltpu.VMEM)
    anywhere = pl.BlockSpec(memory_space=pl.ANY)
    sems = pltpu.SemaphoreType.DMA((n_ep,))
    return pl.pallas_call(
        functools.partial(project_kernel, n_ep),
        out_shape=(
            jax.ShapeDtypeStruct((rows, 4 * cols), jnp.float32),
            jax.ShapeDtypeStruct((rows, gate_w.shape[1]), jnp.float32),
        ),
        in_specs=[vmem, vmem] + [anywhere] * 4,
        out_specs=(vmem, vmem),
        scratch_shapes=[
            pltpu.VMEM((4, depth, cols), jnp.bfloat16),
            pltpu.VMEM((n_ep, rows, depth), jnp.bfloat16),
            pltpu.VMEM((n_ep, rows, 2 * cols), jnp.bfloat16),
            pltpu.VMEM((n_ep, rows, 2 * cols), jnp.bfloat16),
            pltpu.VMEM((n_ep, rows, 2 * cols), jnp.float32),
            pltpu.VMEM((n_ep, rows, 2 * cols), jnp.float32),
            pltpu.VMEM((n_ep, rows, gate_w.shape[1]), jnp.float32),
            pltpu.VMEM((n_ep, rows, gate_w.shape[1]), jnp.float32),
            pltpu.SemaphoreType.DMA((4,)),
        ]
        + [sems] * 8,
        compiler_params=pltpu.CompilerParams(collective_id=0, has_side_effects=True),
        name="project",
    )(hidden, gate_w, wq, wk, wv, wo)


def cell_kernel(proj, keep_ref, write_ref, gain_ref, mem_ref, mixed_ref, mem_out):
    heads = mem_ref.shape[1]
    queries = proj[0, 0:heads]
    keys = proj[0, heads : 2 * heads] * DH ** (-0.5)
    values = proj[0, 2 * heads : 3 * heads]
    out_pre = proj[0, 3 * heads : 4 * heads]
    keep = keep_ref[0]
    write = write_ref[0]
    write_keys = keys * write
    read_old = jnp.zeros_like(queries)
    for d in range(DH):
        block = mem_ref[0, :, d * DH : (d + 1) * DH]
        read_old += queries[:, d : d + 1] * block
        mem_out[0, :, d * DH : (d + 1) * DH] = keep * block + write_keys[:, d : d + 1] * values
    scores = jnp.sum(queries * keys, -1, keepdims=True) * write
    readout = scores * values + keep * read_old
    scaled = readout * lax.rsqrt(jnp.mean(readout * readout, -1, keepdims=True) + 1e-06)
    mixed_ref[0] = (scaled * gain_ref[...] * jax.nn.sigmoid(out_pre)).astype(jnp.bfloat16)


def cell(proj, keep, write, gain, memory):
    rows, heads, flat = memory.shape
    one = lambda *dims: pl.BlockSpec((1,) + dims, lambda b: (b,) + (0,) * len(dims))
    return pl.pallas_call(
        cell_kernel,
        grid=(rows,),
        out_shape=(
            jax.ShapeDtypeStruct((rows, heads, DH), jnp.bfloat16),
            jax.ShapeDtypeStruct((rows, heads, flat), jnp.float32),
        ),
        in_specs=[
            one(4 * heads, DH),
            one(heads, DH),
            one(heads, DH),
            pl.BlockSpec((heads, DH), lambda b: (0, 0)),
            one(heads, flat),
        ],
        out_specs=(one(heads, DH), one(heads, flat)),
        name="cell",
    )(proj, keep, write, gain, memory)


def moe_kernel(
    n_ep,
    n_tp,
    groups,
    mixed,
    hidden,
    gain1,
    gain2,
    router_t,
    route,
    perm,
    perm_t,
    w_out,
    w_gate,
    w_up,
    w_down,
    out_ref,
    wo_buf,
    wg_buf,
    wu_buf,
    wd_buf,
    mix_send,
    mix_recv,
    mid_buf,
    arrived,
    down_send,
    down_recv,
    ret_send,
    ret_recv,
    stat_send,
    stat_recv,
    load_sem,
    m_send,
    m_recv,
    a_send,
    a_recv,
    d_send,
    d_recv,
    r_send,
    r_recv,
    s_send,
    s_recv,
):
    me = lax.axis_index("ep")
    tp = lax.axis_index("tp")
    rows, width = hidden.shape
    share = width // n_tp
    block = rows // groups
    loads = [
        pltpu.make_async_copy(w_out, wo_buf, load_sem.at[0]),
        pltpu.make_async_copy(w_gate.at[0], wg_buf, load_sem.at[1]),
        pltpu.make_async_copy(w_up.at[0], wu_buf, load_sem.at[2]),
        pltpu.make_async_copy(w_down.at[0], wd_buf, load_sem.at[3]),
    ]
    for load in loads:
        load.start()
    ep_after = [(lax.rem(me + o, n_ep), tp) for o in range(n_ep)]
    ep_before = [(lax.rem(me + n_ep - o, n_ep), tp) for o in range(n_ep)]
    tp_after = [(me, lax.rem(tp + o, n_tp)) for o in range(n_tp)]
    greet(ep_after[1:] + tp_after[1:])
    started = []

    def begin(copies):
        for copy in copies:
            copy.start()
        started.extend(copies)
        return copies

    mixed_sorted = jnp.dot(perm[...], mixed[...], preferred_element_type=jnp.float32).astype(jnp.bfloat16)
    loads[0].wait()
    for c in range(n_tp):
        columns = slice(c * share, (c + 1) * share)
        mix_send[:, columns] = jnp.dot(
            mixed_sorted, wo_buf[:, columns], preferred_element_type=jnp.float32
        ).astype(jnp.bfloat16)
    copies = begin(
        [remote(mix_send, mix_recv.at[o], m_send.at[o], m_recv.at[o], tp_after[o]) for o in range(1, n_tp)]
    )
    joined = res_alpha * jnp.dot(perm[...], hidden[...], preferred_element_type=jnp.float32)
    joined += mix_send[...].astype(jnp.float32)
    for o in range(1, n_tp):
        copies[o - 1].wait_recv()
        joined += mix_recv[o].astype(jnp.float32)
    mid_float = layer_norm(joined, gain1[...])
    for g in range(groups):
        mid_buf[g] = mid_float[g * block : (g + 1) * block].astype(jnp.bfloat16)
    copies = begin(
        [
            remote(
                mid_buf.at[lax.div(ep_after[o][0], GROUP_SIZE)],
                arrived.at[o],
                a_send.at[o],
                a_recv.at[o],
                ep_after[o],
            )
            for o in range(1, n_ep)
        ]
    )
    high = mid_float.astype(jnp.bfloat16)
    rest = mid_float - high.astype(jnp.float32)
    middle = rest.astype(jnp.bfloat16)
    low = (rest - middle.astype(jnp.float32)).astype(jnp.bfloat16)
    logits = jnp.zeros((rows, router_t.shape[0]), jnp.float32)
    for piece in (low, middle, high):
        logits += lax.dot_general(
            piece, router_t[...], (((1,), (1,)), ((), ())), preferred_element_type=jnp.float32
        )
    first = route[:, 0:1]
    second = route[:, 1:2]
    lanes = lax.broadcasted_iota(jnp.int32, logits.shape, 1)
    pick = lambda index: jnp.sum(jnp.where(lanes == index, logits, 0.0), -1, keepdims=True)
    first_logit = pick(first)
    second_logit = pick(second)
    group_gate = jax.nn.sigmoid(pick(n_ep + lax.shift_right_logical(first, 2)))
    weight1 = group_gate * jax.nn.sigmoid(first_logit - second_logit)
    weight2 = group_gate * jax.nn.sigmoid(second_logit - first_logit)
    arrived[0] = mid_buf[lax.div(me, GROUP_SIZE)]
    loads[1].wait()
    loads[2].wait()
    for copy in copies:
        copy.wait_recv()
    tokens = arrived[...].astype(jnp.float32).reshape(n_ep * block, width).astype(jnp.bfloat16)
    gate_pre = jnp.dot(tokens, wg_buf[...], preferred_element_type=jnp.float32)
    up_pre = jnp.dot(tokens, wu_buf[...], preferred_element_type=jnp.float32)
    units = (gate_pre * jax.nn.sigmoid(gate_pre) * up_pre).astype(jnp.bfloat16)
    loads[3].wait()
    copies = []
    for o in list(range(1, n_tp)) + [0]:
        columns = pl.ds(pl.multiple_of(tp_after[o][1] * share, share), share)
        down_send[o] = jnp.dot(units, wd_buf[:, columns], preferred_element_type=jnp.float32).astype(
            jnp.bfloat16
        )
        if o:
            copies += begin(
                [remote(down_send.at[o], down_recv.at[o], d_send.at[o], d_recv.at[o], tp_after[o])]
            )
    total = down_send[0].astype(jnp.float32)
    for o in range(1, n_tp):
        copies[o - 1].wait_recv()
        total += down_recv[o].astype(jnp.float32)
    for o in range(n_ep):
        ret_send[o] = total[o * block : (o + 1) * block].astype(jnp.bfloat16)
    copies = begin(
        [
            remote(ret_send.at[o], ret_recv.at[o], r_send.at[o], r_recv.at[o], ep_before[o])
            for o in range(1, n_ep)
        ]
    )
    mine = pl.ds(pl.multiple_of(tp * share, share), share)
    joined = res_alpha * mid_buf[:, :, mine].astype(jnp.float32).reshape(rows, share)
    for o in range(n_ep):
        expert = ep_after[o][0]
        if o:
            copies[o - 1].wait_recv()
        result = (ret_recv[o] if o else ret_send[0]).astype(jnp.float32)
        weight = jnp.where(first == expert, weight1, 0.0) + jnp.where(second == expert, weight2, 0.0)
        joined += weight * jnp.concatenate([result] * groups, 0)
    row_sum = jnp.sum(joined, -1, keepdims=True)
    square_sum = jnp.sum(joined * joined, -1, keepdims=True)
    stat_send[0] = jnp.broadcast_to(row_sum, stat_send.shape[1:])
    stat_send[1] = jnp.broadcast_to(square_sum, stat_send.shape[1:])
    copies = begin(
        [remote(stat_send, stat_recv.at[o], s_send.at[o], s_recv.at[o], tp_after[o]) for o in range(1, n_tp)]
    )
    for o in range(1, n_tp):
        copies[o - 1].wait_recv()
        row_sum += stat_recv[o, 0][:, 0:1]
        square_sum += stat_recv[o, 1][:, 0:1]
    row_mean = row_sum / width
    row_var = square_sum / width - row_mean * row_mean
    result = ((joined - row_mean) * lax.rsqrt(row_var + 1e-05) * gain2[...]).astype(jnp.bfloat16)
    out_ref[...] = jnp.dot(perm_t[...], result, preferred_element_type=jnp.float32).astype(jnp.bfloat16)
    for copy in started:
        copy.wait_send()


def mix_and_moe(n_ep, n_tp, groups, *operands):
    mixed, hidden = operands[:2]
    w_out, w_gate, w_up, w_down = operands[-4:]
    rows, width = hidden.shape
    share = width // n_tp
    block = rows // groups
    vmem = pl.BlockSpec(memory_space=pltpu.VMEM)
    anywhere = pl.BlockSpec(memory_space=pl.ANY)
    ep_sems = pltpu.SemaphoreType.DMA((n_ep,))
    tp_sems = pltpu.SemaphoreType.DMA((n_tp,))
    half = jnp.bfloat16
    return pl.pallas_call(
        functools.partial(moe_kernel, n_ep, n_tp, groups),
        out_shape=jax.ShapeDtypeStruct((rows, share), half),
        in_specs=[vmem] * (len(operands) - 4) + [anywhere] * 4,
        out_specs=vmem,
        scratch_shapes=[
            pltpu.VMEM(w_out.shape, half),
            pltpu.VMEM(w_gate.shape[1:], half),
            pltpu.VMEM(w_up.shape[1:], half),
            pltpu.VMEM(w_down.shape[1:], half),
            pltpu.VMEM((rows, width), half),
            pltpu.VMEM((n_tp, rows, width), half),
            pltpu.VMEM((groups, block, width), half),
            pltpu.VMEM((n_ep, block, width), half),
            pltpu.VMEM((n_tp, n_ep * block, share), half),
            pltpu.VMEM((n_tp, n_ep * block, share), half),
            pltpu.VMEM((n_ep, block, share), half),
            pltpu.VMEM((n_ep, block, share), half),
            pltpu.VMEM((2, rows, DH), jnp.float32),
            pltpu.VMEM((n_tp, 2, rows, DH), jnp.float32),
            pltpu.SemaphoreType.DMA((4,)),
            tp_sems,
            tp_sems,
            ep_sems,
            ep_sems,
            tp_sems,
            tp_sems,
            ep_sems,
            ep_sems,
            tp_sems,
            tp_sems,
        ],
        compiler_params=pltpu.CompilerParams(collective_id=1, has_side_effects=True),
        name="mix_and_moe",
    )(*operands)


def kernel_body(
    hidden_in,
    w_query,
    w_key,
    w_value,
    w_outgate,
    w_igate,
    w_fgate,
    input_bias,
    forget_bias,
    mem_state,
    max_state,
    head_gain,
    w_output,
    first_gain,
    w_group_router,
    w_expert_router,
    expert_route,
    w_expgate,
    w_expup,
    w_expdown,
    second_gain,
):
    n_ep, n_tp = lax.axis_size("ep"), lax.axis_size("tp")
    rows, width = hidden_in.shape
    heads = mem_state.shape[1]
    groups = w_group_router.shape[1]
    gate_w = jnp.concatenate([w_igate, w_fgate], 1)
    gate_w = jnp.pad(gate_w, ((0, 0), (0, DH - 2 * heads)))
    projected, gate_sums = project(n_ep, hidden_in, gate_w, w_query, w_key, w_value, w_outgate)
    log_input = gate_sums[:, :heads] + input_bias
    log_forget = jax.nn.log_sigmoid(gate_sums[:, heads : 2 * heads] + forget_bias)
    new_max = jnp.maximum(log_forget + max_state, log_input)
    keep_old = jnp.exp(log_forget + max_state - new_max)
    write_new = jnp.exp(log_input - new_max)
    spread_gate = lambda gate: jnp.broadcast_to(gate[:, :, None], (rows, heads, DH))
    mixed, memory_next = cell(
        projected.reshape(rows, 4 * heads, DH),
        spread_gate(keep_old),
        spread_gate(write_new),
        head_gain.reshape(heads, DH),
        mem_state,
    )
    row_ids = jnp.arange(rows, dtype=jnp.int32)
    group = expert_route[:, 0] // GROUP_SIZE
    earlier = (group[:, None] == group[None, :]) & (row_ids[None, :] < row_ids[:, None])
    place = group * (rows // groups) + jnp.sum(earlier.astype(jnp.int32), 1)
    perm = place[None, :] == row_ids[:, None]
    route = jnp.sum(jnp.where(perm[:, :, None], expert_route[None], 0), 1)
    router = jnp.concatenate([w_expert_router, w_group_router], 1)
    router_t = jnp.pad(router, ((0, 0), (0, -router.shape[1] % 16))).T
    hidden_out = mix_and_moe(
        n_ep,
        n_tp,
        groups,
        mixed.reshape(rows, heads * DH),
        hidden_in,
        first_gain[None],
        second_gain[None],
        router_t,
        route,
        perm.astype(jnp.bfloat16),
        perm.T.astype(jnp.bfloat16),
        w_output,
        w_expgate,
        w_expup,
        w_expdown,
    )
    return (hidden_out, memory_next, new_max)


def either_body(*operands):
    hidden_in, w_query, group_router, experts = operands[0], operands[1], operands[14], operands[17]
    rows, width = hidden_in.shape
    block, odd_rows = divmod(rows, group_router.shape[1])
    aligned = rows % 16 == 0 and block % 8 == 0 and odd_rows == 0 and experts.shape[0] == 1
    aligned = aligned and w_query.shape[0] % DH == 0 and width // lax.axis_size("tp") % DH == 0
    return (kernel_body if aligned else body)(*operands)


def solution(mesh):
    return jax.shard_map(
        either_body,
        mesh=mesh,
        in_specs=(
            P("ep", None),
            P("ep", "tp"),
            P("ep", "tp"),
            P("ep", "tp"),
            P("ep", "tp"),
            P("ep", "tp"),
            P("ep", "tp"),
            P("tp"),
            P("tp"),
            P("ep", "tp", None),
            P("ep", "tp"),
            P("tp"),
            P("tp", None),
            P(),
            P(),
            P(),
            P("ep", None),
            P("ep", None, "tp"),
            P("ep", None, "tp"),
            P("ep", "tp", None),
            P("tp"),
        ),
        out_specs=(P("ep", "tp"), P("ep", "tp", None), P("ep", "tp")),
        check_vma=False,
    )
```
